32 devices in a mesh: rep: 4 (over z), fs: 4 (over y, x), tp: 2 (over core).
Axes of the slice: x: 2, y: 2, z: 4, core: 2. Of those that a mesh axis runs over, the one named last changes fastest.
Arguments:
- gate_pre: bfloat16 [2560, 2816], P(('rep', 'fs'), 'tp'), may hold values from -6 to 6
- up_pre: bfloat16 [2560, 2816], P(('rep', 'fs'), 'tp'), may hold values from -6 to 6
- gate_taps: bfloat16 [3, 2816], P(None, 'tp'), may hold values from -3 to 3
- up_taps: bfloat16 [3, 2816], P(None, 'tp'), may hold values from -3 to 3
- down_weight: bfloat16 [2816, 2048], P('tp', 'fs'), may hold values from -0.125 to 0.125
- cotangent: bfloat16 [2560, 2048], P('rep', 'fs'), may hold values from -6 to 6
Outputs:
- grad_gate: bfloat16 [2560, 2816], P(('rep', 'fs'), 'tp')
- grad_up: bfloat16 [2560, 2816], P(('rep', 'fs'), 'tp')
- grad_gate_taps: float32 [3, 2816], P(None, 'tp')
- grad_up_taps: float32 [3, 2816], P(None, 'tp')
- grad_down: float32 [4, 512, 2816], P('fs', 'rep', 'tp')
- down_norms: float32 [2816], P('tp')
The draws below stay inside these ranges and needn't reach their ends.
All inputs are finite; a program needn't handle non-finite values.
Results may differ from the reference program's by a relative error of at most 0.0049.
Values may be sent and summed in bfloat16 or wider, within the bound.
A program may use at most 64 MiB of HBM per device.

```python
import jax
import jax.numpy as jnp
from jax import lax

D = 2048
FF = 2816
TOK_DEV = 160
TOKENS = 2560
N_REP = 4
N_FS = 4


def raised(values, own_key, source, target, shards_of, factor):
    def block_of(dim):
        return (jnp.arange(values.shape[dim]) // (values.shape[dim] // shards_of)).reshape((-1,) + (1,) * (values.ndim - 1 - dim))

    one_side = jax.random.permutation(own_key, shards_of)[block_of(target)]
    other_side = (block_of(target) + shards_of // 2) % shards_of
    return jnp.where((block_of(source) == one_side) | (block_of(source) == other_side), factor * values, values)


def levels(stream_key, extent, shards, least, high):
    level = 1.0
    for axis_at, shards_of in shards:
        steps = jax.random.uniform(jax.random.fold_in(jax.random.fold_in(stream_key, 6), axis_at), (shards_of,), jnp.float32, least / len(shards), high / len(shards))
        level = level * jnp.repeat(jnp.exp(steps), extent[axis_at] // shards_of).reshape((-1,) + (1,) * (len(extent) - 1 - axis_at))
    return level


def normal_values(rng, shape, spread, reach, pieces=(), held_as=jnp.bfloat16):
    array = jax.random.normal(rng, shape, jnp.float32) * spread
    if len(pieces) > 0:
        array = levels(rng, shape, pieces, -0.22, 0.18) * array
    return jnp.clip(array, min=-reach, max=reach).astype(held_as)


def gaussian_with(key, extent, scale, bound, pieces, heavy, kind=jnp.bfloat16):
    result = scale * jax.random.normal(key, extent, jnp.float32)
    if pieces:
        result = result * levels(key, extent, pieces, -0.22, 0.18)
    return jnp.clip(raised(result, jax.random.fold_in(key, 3), *heavy), -bound, bound).astype(kind)


def setup_inputs(seed: int = 0) -> dict:
    seeds = jax.random.split(jax.random.key(seed), 7)
    gate_pre = normal_values(seeds[0], (TOKENS, FF), 1.0, 6.0, ((0, 16), (1, 2)))
    up_pre = normal_values(seeds[1], (TOKENS, FF), 1.0, 6.0, ((0, 16), (1, 2)))
    gate_taps = normal_values(seeds[2], (3, FF), 0.6, 3.0, ((1, 2),))
    up_taps = normal_values(seeds[3], (3, FF), 0.6, 3.0, ((1, 2),))
    down_weight = normal_values(seeds[4], (FF, D), D ** -0.5, 0.125, ((0, 2), (1, 4)))
    cotangent = gaussian_with(seeds[5], (TOKENS, D), 1.0, 6.0, ((0, 4), (1, 4)), (0, 1, 4, 2.0))
    return {"gate_pre": gate_pre, "up_pre": up_pre, "gate_taps": gate_taps, "up_taps": up_taps, "down_weight": down_weight, "cotangent": cotangent}


def shift_conv(padded, tap_coef):
    return tap_coef[0] * padded[:, :-2] + tap_coef[1] * padded[:, 1:-1] + tap_coef[2] * padded[:, 2:]


def back_conv(padded, tap_coef):
    return tap_coef[2] * padded[:, :-2] + tap_coef[1] * padded[:, 1:-1] + tap_coef[0] * padded[:, 2:]


def reference(gate_pre, up_pre, gate_taps, up_taps, down_weight, cotangent):
    length = TOK_DEV * N_FS
    width = gate_pre.shape[1]
    gate_pad = jnp.pad(gate_pre.astype(jnp.float32).reshape(N_REP, length, width), ((0, 0), (2, 0), (0, 0)))
    up_pad = jnp.pad(up_pre.astype(jnp.float32).reshape(N_REP, length, width), ((0, 0), (2, 0), (0, 0)))
    gate_coef = gate_taps.astype(jnp.float32)
    up_coef = up_taps.astype(jnp.float32)
    gate_conv = shift_conv(gate_pad, gate_coef)
    up_conv = shift_conv(up_pad, up_coef)
    gate_sig = jax.nn.sigmoid(gate_conv)
    activated = gate_conv * gate_sig
    hidden = (activated * up_conv).astype(jnp.bfloat16).reshape(TOKENS, width)
    quarter = D // N_FS
    d_hidden = jnp.zeros((TOKENS, width), jnp.float32)
    for index in range(N_FS):
        part_sum = lax.dot_general(cotangent[:, index * quarter:(index + 1) * quarter],
                                   down_weight[:, index * quarter:(index + 1) * quarter],
                                   (((1,), (1,)), ((), ())), preferred_element_type=jnp.float32)
        rounded = lax.optimization_barrier(part_sum.astype(jnp.bfloat16))
        d_hidden = d_hidden + rounded.astype(jnp.float32)
    d_hidden = d_hidden.reshape(N_REP, length, width)
    d_gate = d_hidden * up_conv * gate_sig * (1.0 + gate_conv * (1.0 - gate_sig))
    d_up = d_hidden * activated
    gate_back = jnp.pad(d_gate, ((0, 0), (0, 2), (0, 0)))
    up_back = jnp.pad(d_up, ((0, 0), (0, 2), (0, 0)))
    grad_gate = back_conv(gate_back, gate_coef).astype(jnp.bfloat16).reshape(TOKENS, width)
    grad_up = back_conv(up_back, up_coef).astype(jnp.bfloat16).reshape(TOKENS, width)
    grad_scale = float(TOKENS) ** -0.5
    grad_gate_taps = jnp.stack([jnp.sum(d_gate * gate_pad[:, offset:offset + length], axis=(0, 1)) for offset in range(3)]) * grad_scale
    grad_up_taps = jnp.stack([jnp.sum(d_up * up_pad[:, offset:offset + length], axis=(0, 1)) for offset in range(3)]) * grad_scale
    grad_full = lax.dot_general(cotangent, hidden, (((0,), (0,)), ((), ())), preferred_element_type=jnp.float32) * grad_scale
    down_norms = jnp.sum(grad_full * grad_full, axis=0) / D
    grad_down = grad_full.reshape(N_FS, quarter, width)
    return grad_gate, grad_up, grad_gate_taps, grad_up_taps, grad_down, down_norms
```

```python
import functools

import jax
import jax.numpy as jnp
from jax import lax
from jax.experimental import pallas as pl
from jax.experimental.pallas import tpu as pltpu
from jax.sharding import PartitionSpec as P

MESH = pl.DeviceIdType.MESH
LANES = 128


def passed_along(array, axis, by):
    count = lax.axis_size(axis)
    pairs = [(i, i + by) for i in range(count) if 0 <= i + by < count]
    return lax.ppermute(array, axis, pairs)


def shift_conv(padded, tap_coef):
    return tap_coef[0] * padded[:-2] + tap_coef[1] * padded[1:-1] + tap_coef[2] * padded[2:]


def back_conv(padded, tap_coef):
    return tap_coef[2] * padded[:-2] + tap_coef[1] * padded[1:-1] + tap_coef[0] * padded[2:]


def local(gate_pre, up_pre, gate_taps, up_taps, down_weight, cotangent):
    tok_rows = gate_pre.shape[0]
    width = gate_pre.shape[1]
    prev_rows = passed_along(jnp.stack([gate_pre[-2:], up_pre[-2:]]), "fs", 1)
    gate_pad = jnp.concatenate([prev_rows[0], gate_pre], 0).astype(jnp.float32)
    up_pad = jnp.concatenate([prev_rows[1], up_pre], 0).astype(jnp.float32)
    gate_coef = gate_taps.astype(jnp.float32)
    up_coef = up_taps.astype(jnp.float32)
    gate_conv = shift_conv(gate_pad, gate_coef)
    up_conv = shift_conv(up_pad, up_coef)
    gate_sig = jax.nn.sigmoid(gate_conv)
    activated = gate_conv * gate_sig
    hidden = (activated * up_conv).astype(jnp.bfloat16)
    partial_rows = lax.dot_general(
        cotangent, down_weight, (((1,), (1,)), ((), ())), preferred_element_type=jnp.float32
    ).astype(jnp.bfloat16)
    received = lax.all_to_all(partial_rows, "fs", split_axis=0, concat_axis=0, tiled=True)
    d_hidden = jnp.sum(received.reshape(-1, tok_rows, width).astype(jnp.float32), axis=0)
    d_gate = d_hidden * up_conv * gate_sig * (1.0 + gate_conv * (1.0 - gate_sig))
    d_up = d_hidden * activated
    next_rows = passed_along(jnp.stack([d_gate[:2], d_up[:2]]), "fs", -1)
    grad_gate = back_conv(jnp.concatenate([d_gate, next_rows[0]], 0), gate_coef).astype(
        jnp.bfloat16
    )
    grad_up = back_conv(jnp.concatenate([d_up, next_rows[1]], 0), up_coef).astype(jnp.bfloat16)
    taps_part = jnp.stack(
        [
            jnp.stack(
                [
                    jnp.sum(d_gate * gate_pad[offset : offset + tok_rows], axis=0)
                    for offset in range(3)
                ]
            ),
            jnp.stack(
                [jnp.sum(d_up * up_pad[offset : offset + tok_rows], axis=0) for offset in range(3)]
            ),
        ]
    )
    grad_scale = float(tok_rows * lax.axis_size("rep") * lax.axis_size("fs")) ** (-0.5)
    folded_sum = lax.dot_general(
        cotangent,
        lax.all_gather(hidden, "fs", axis=0, tiled=True),
        (((0,), (0,)), ((), ())),
        preferred_element_type=jnp.float32,
    )
    grad_share = lax.psum_scatter(folded_sum, "rep", scatter_dimension=0, tiled=True)
    grad_share = grad_share * grad_scale
    norm_part = jnp.sum(grad_share * grad_share, axis=0)
    norm_total, taps_total = lax.psum((norm_part, taps_part), ("rep", "fs"))
    return (
        grad_gate,
        grad_up,
        taps_total[0] * grad_scale,
        taps_total[1] * grad_scale,
        grad_share[None],
        norm_total / (cotangent.shape[1] * lax.axis_size("fs")),
    )


HALO = 16
FS_MASKS = ((1, 2), (2, 1))
REP_MASKS = ((1, 2), (1, 2))


def flip(v, mask):
    if mask == 1:
        return v + 1 - 2 * (v % 2)
    if mask == 2:
        return (v + 2) % 4
    return 3 - v


def column_chunks(width):
    tiles = width // LANES
    widths = [1, 1, 2, 2]
    rest = tiles - sum(widths)
    if rest < 2:
        widths, rest = [], tiles
    widths = widths + [rest // 2, rest - rest // 2] if rest > 1 else [rest]
    chunks, at = [], 0
    for tiles_here in widths:
        chunks.append((at * LANES, tiles_here * LANES))
        at += tiles_here
    return chunks


def kernel(
    scale, model_width, gate_hbm, up_hbm, gtaps_hbm, utaps_hbm, weight_hbm, cot_hbm,
    grad_gate, grad_up, gtaps_out, utaps_out, grad_down, norms_out,
    gate, up, gtaps, utaps, weight, cot, cot_t, halo, gate_pad, up_pad, coef_gate, coef_up,
    hid, parts, rs1, rs2, rs_out, prod, prod_out, zs1, zs2, z_out, dg_pad, du_pad,
    dhalo_out, dhalo_in, taps_out1, taps_in1, taps_out2, taps_in2,
    norm_out1, norm_in1, norm_out2, norm_in2, load_sem, send_sem, recv_sem,
):
    f = lax.axis_index("fs")
    r = lax.axis_index("rep")
    rows, width = gate.shape
    blk = grad_down.shape[0]
    chunks = column_chunks(width)
    n = len(chunks)
    sends = []

    loads = []
    for i, (src, dst) in enumerate((
        (gate_hbm, gate), (up_hbm, up), (cot_hbm, cot), (weight_hbm, weight),
        (gtaps_hbm, gtaps), (utaps_hbm, utaps),
    )):
        copy = pltpu.make_async_copy(src, dst, load_sem.at[i])
        copy.start()
        loads.append(copy)

    barrier = pltpu.get_barrier_semaphore()
    for d in (1, 2, 3):
        pl.semaphore_signal(barrier, inc=1, device_id={"fs": (f + d) % 4}, device_id_type=MESH)
        pl.semaphore_signal(barrier, inc=1, device_id={"rep": (r + d) % 4}, device_id_type=MESH)
    pl.semaphore_wait(barrier, 6)

    def push(src, dst, axis, to):
        k = len(sends)
        copy = pltpu.make_async_remote_copy(
            src_ref=src, dst_ref=dst, send_sem=send_sem.at[k], recv_sem=recv_sem.at[k],
            device_id={axis: to}, device_id_type=MESH,
        )
        copy.start()
        sends.append(copy)
        return copy

    def cols(c):
        return pl.ds(chunks[c][0], chunks[c][1])

    def tile_list(c):
        return [pl.ds(at, LANES) for at in range(chunks[c][0], chunks[c][0] + chunks[c][1], LANES)]

    loads[0].wait()
    loads[1].wait()
    nxt = (f + 1) % 4
    halo_in = [
        push(gate.at[pl.ds(rows - HALO, HALO)], halo.at[0], "fs", nxt),
        push(up.at[pl.ds(rows - HALO, HALO)], halo.at[1], "fs", nxt),
    ]

    def part(c):
        product = lax.dot_general(
            cot[...], weight[cols(c), :], (((1,), (1,)), ((), ())),
            preferred_element_type=jnp.float32,
        )
        parts[:, :, cols(c)] = product.astype(jnp.bfloat16).reshape(4, rows, chunks[c][1])

    rs1_in, rs2_in, ag1_in, ag2_in, z1_in, z2_in = {}, {}, {}, {}, {}, {}

    def rs_first(c):
        m1, m2 = FS_MASKS[c % 2]
        to = flip(f, m1)
        rs1_in[c] = [
            push(parts.at[flip(to, m2), :, cols(c)], rs1.at[1, :, cols(c)], "fs", to),
            push(parts.at[to, :, cols(c)], rs1.at[0, :, cols(c)], "fs", to),
        ]

    def rs_second(c):
        m1, m2 = FS_MASKS[c % 2]
        to = flip(f, m2)
        rs1_in[c][0].wait_recv()
        for t in tile_list(c):
            rs_out[:, t] = (
                parts[to, :, t].astype(jnp.float32) + rs1[1, :, t].astype(jnp.float32)
            ).astype(jnp.bfloat16)
        rs2_in[c] = push(rs_out.at[:, cols(c)], rs2.at[:, cols(c)], "fs", to)

    def hidden(c):
        for t in tile_list(c):
            gc = [gtaps[k : k + 1, t].astype(jnp.float32) for k in range(3)]
            uc = [utaps[k : k + 1, t].astype(jnp.float32) for k in range(3)]
            g_conv = sum(gc[k] * gate_pad[pl.ds(6 + k, rows), t] for k in range(3))
            u_conv = sum(uc[k] * up_pad[pl.ds(6 + k, rows), t] for k in range(3))
            sig = jax.nn.sigmoid(g_conv)
            act = g_conv * sig
            hid[f, :, t] = (act * u_conv).astype(jnp.bfloat16)
            coef_up[:, t] = act
            coef_gate[:, t] = u_conv * sig * (1.0 + g_conv * (1.0 - sig))
        m1, m2 = FS_MASKS[c % 2]
        ag1_in[c] = push(hid.at[f, :, cols(c)], hid.at[f, :, cols(c)], "fs", flip(f, m1))

    def ag_second(c):
        m1, m2 = FS_MASKS[c % 2]
        to = flip(f, m2)
        own = push(hid.at[f, :, cols(c)], hid.at[f, :, cols(c)], "fs", to)
        ag1_in[c].wait_recv()
        slot = flip(f, m1)
        ag2_in[c] = [own, push(hid.at[slot, :, cols(c)], hid.at[slot, :, cols(c)], "fs", to)]

    def product(c):
        for copy in ag2_in[c]:
            copy.wait_recv()
        result = jnp.dot(
            cot_t[...], hid[:, :, cols(c)].reshape(4 * rows, chunks[c][1]),
            preferred_element_type=jnp.float32,
        ).reshape(4, blk, chunks[c][1])
        prod[:, :, cols(c)] = result
        prod_out[:, :, cols(c)] = result.astype(jnp.bfloat16)
        m1, m2 = REP_MASKS[c % 2]
        to = flip(r, m1)
        z1_in[c] = [
            push(prod_out.at[flip(to, m2), :, cols(c)], zs1.at[1, :, cols(c)], "rep", to),
            push(prod_out.at[to, :, cols(c)], zs1.at[0, :, cols(c)], "rep", to),
        ]

    def z_second(c):
        m1, m2 = REP_MASKS[c % 2]
        to = flip(r, m2)
        z1_in[c][0].wait_recv()
        for t in tile_list(c):
            z_out[:, t] = (prod[to, :, t] + zs1[1, :, t].astype(jnp.float32)).astype(jnp.bfloat16)
        z2_in[c] = push(z_out.at[:, cols(c)], zs2.at[:, cols(c)], "rep", to)

    def z_last(c):
        z1_in[c][1].wait_recv()
        z2_in[c].wait_recv()
        for t in tile_list(c):
            total = (
                prod[r, :, t] + zs1[0, :, t].astype(jnp.float32) + zs2[:, t].astype(jnp.float32)
            ) * scale
            grad_down[:, t] = total
            norm_out1[:, t] = jnp.sum(total * total, axis=0, keepdims=True)

    def rs_last(c):
        rs1_in[c][1].wait_recv()
        rs2_in[c].wait_recv()
        for t in tile_list(c):
            dh = (
                parts[f, :, t].astype(jnp.float32)
                + rs1[0, :, t].astype(jnp.float32)
                + rs2[:, t].astype(jnp.float32)
            )
            d_gate = dh * coef_gate[:, t]
            d_up = dh * coef_up[:, t]
            dg_pad[pl.ds(0, rows), t] = d_gate
            du_pad[pl.ds(0, rows), t] = d_up
            dhalo_out[0:2, t] = d_gate[0:2]
            dhalo_out[2:4, t] = d_up[0:2]
            for k in range(3):
                taps_out1[k : k + 1, t] = jnp.sum(
                    d_gate * gate_pad[pl.ds(6 + k, rows), t], axis=0, keepdims=True
                )
                taps_out1[3 + k : 4 + k, t] = jnp.sum(
                    d_up * up_pad[pl.ds(6 + k, rows), t], axis=0, keepdims=True
                )

    def spread(src, landing, axis, me):
        return [push(src, landing.at[me], axis, (me + d) % 4) for d in (1, 2, 3)]

    def gather_sum(copies, own, landing, me):
        for copy in copies:
            copy.wait_recv()
        landing[me] = own[...]
        return (landing[0] + landing[1]) + (landing[2] + landing[3])

    loads[2].wait()
    loads[3].wait()
    part(0)
    rs_first(0)
    part(1)
    rs_first(1)
    gate_pad[pl.ds(8, rows), :] = gate[...].astype(jnp.float32)
    up_pad[pl.ds(8, rows), :] = up[...].astype(jnp.float32)
    taps_out1[...] = jnp.zeros_like(taps_out1)
    dhalo_out[...] = jnp.zeros_like(dhalo_out)
    loads[4].wait()
    loads[5].wait()
    for copy in halo_in:
        copy.wait_recv()
    inner = (f > 0).astype(jnp.float32)
    gate_pad[6:8, :] = halo[0].astype(jnp.float32)[HALO - 2 :] * inner
    up_pad[6:8, :] = halo[1].astype(jnp.float32)[HALO - 2 :] * inner

    hidden(0)
    hidden(1)
    hidden(2)
    hidden(3)
    ag_second(0)
    ag_second(1)
    cot_t[...] = cot[...].T
    hidden(4)
    hidden(5)
    ag_second(2)
    ag_second(3)
    part(2)
    part(3)
    product(0)
    product(1)
    ag_second(4)
    ag_second(5)
    rs_first(2)
    rs_first(3)
    part(4)
    part(5)
    product(2)
    product(3)
    z_second(0)
    z_second(1)
    rs_second(0)
    rs_second(1)
    rs_first(4)
    rs_first(5)
    product(4)
    product(5)
    z_second(2)
    z_second(3)
    rs_second(2)
    rs_second(3)
    z_last(0)
    z_last(1)
    rs_last(0)
    rs_last(1)
    rs_second(4)
    rs_second(5)
    rs_last(2)
    rs_last(3)
    z_second(4)
    z_second(5)
    z_last(2)
    z_last(3)
    rs_last(4)
    rs_last(5)
    taps1 = spread(taps_out1, taps_in1, "fs", f)
    dhalo = push(dhalo_out, dhalo_in, "fs", (f + 3) % 4)
    z_last(4)
    z_last(5)
    norm1 = spread(norm_out1, norm_in1, "fs", f)
    taps_out2[...] = gather_sum(taps1, taps_out1, taps_in1, f)
    taps2 = spread(taps_out2, taps_in2, "rep", r)
    norm_out2[...] = gather_sum(norm1, norm_out1, norm_in1, f)
    norm2 = spread(norm_out2, norm_in2, "rep", r)
    dhalo.wait_recv()
    inner = (f < 3).astype(jnp.float32)
    dg_pad[rows : rows + 2, :] = dhalo_in[0:2, :] * inner
    du_pad[rows : rows + 2, :] = dhalo_in[2:4, :] * inner
    for c in range(n):
        for t in tile_list(c):
            for taps, pad, out in ((gtaps, dg_pad, grad_gate), (utaps, du_pad, grad_up)):
                out[:, t] = sum(
                    taps[2 - k : 3 - k, t].astype(jnp.float32) * pad[pl.ds(k, rows), t]
                    for k in range(3)
                ).astype(jnp.bfloat16)
    taps_total = gather_sum(taps2, taps_out2, taps_in2, r) * scale
    gtaps_out[...] = taps_total[0:3]
    utaps_out[...] = taps_total[3:6]
    norms_out[...] = gather_sum(norm2, norm_out2, norm_in2, r) * (1.0 / model_width)
    for copy in sends:
        copy.wait_send()


def fused(gate_pre, up_pre, gate_taps, up_taps, down_weight, cotangent):
    rows, width = gate_pre.shape
    if rows % 16 or width % LANES or width // LANES < 8 or cotangent.shape[1] % 64:
        return local(gate_pre, up_pre, gate_taps, up_taps, down_weight, cotangent)
    depth = cotangent.shape[1]
    blk = depth // lax.axis_size("rep")
    scale = float(rows * lax.axis_size("rep") * lax.axis_size("fs")) ** (-0.5)
    model_width = depth * lax.axis_size("fs")
    f32, bf16 = jnp.float32, jnp.bfloat16
    vmem = pltpu.VMEM
    shapes = [
        ((rows, width), bf16), ((rows, width), bf16), ((3, width), bf16), ((3, width), bf16),
        ((width, depth), bf16), ((4 * rows, depth), bf16), ((depth, 4 * rows), bf16),
        ((2, HALO, width), bf16), ((rows + 8, width), f32), ((rows + 8, width), f32),
        ((rows, width), f32), ((rows, width), f32),
        ((4, rows, width), bf16), ((4, rows, width), bf16), ((2, rows, width), bf16),
        ((rows, width), bf16), ((rows, width), bf16),
        ((4, blk, width), f32), ((4, blk, width), bf16), ((2, blk, width), bf16),
        ((blk, width), bf16), ((blk, width), bf16), ((rows + 8, width), f32),
        ((rows + 8, width), f32), ((8, width), f32), ((8, width), f32),
        ((8, width), f32), ((4, 8, width), f32), ((8, width), f32), ((4, 8, width), f32),
        ((1, width), f32), ((4, 1, width), f32), ((1, width), f32), ((4, 1, width), f32),
    ]
    outs = pl.pallas_call(
        functools.partial(kernel, scale, model_width),
        out_shape=[
            jax.ShapeDtypeStruct((rows, width), bf16), jax.ShapeDtypeStruct((rows, width), bf16),
            jax.ShapeDtypeStruct((3, width), f32), jax.ShapeDtypeStruct((3, width), f32),
            jax.ShapeDtypeStruct((blk, width), f32), jax.ShapeDtypeStruct((1, width), f32),
        ],
        in_specs=[pl.BlockSpec(memory_space=pl.ANY)] * 6,
        out_specs=[pl.BlockSpec(memory_space=pltpu.VMEM)] * 6,
        scratch_shapes=[vmem(shape, kind) for shape, kind in shapes] + [
            pltpu.SemaphoreType.DMA((6,)), pltpu.SemaphoreType.DMA((96,)),
            pltpu.SemaphoreType.DMA((96,)),
        ],
        compiler_params=pltpu.CompilerParams(
            collective_id=0, has_side_effects=True, vmem_limit_bytes=56 * 1024 * 1024
        ),
    )(gate_pre, up_pre, gate_taps, up_taps, down_weight, cotangent)
    return outs[0], outs[1], outs[2], outs[3], outs[4][None], outs[5][0]


def solution(mesh):
    return jax.shard_map(
        fused if mesh.shape["fs"] == 4 and mesh.shape["rep"] == 4 else local,
        mesh=mesh,
        in_specs=(
            P(("rep", "fs"), "tp"),
            P(("rep", "fs"), "tp"),
            P(None, "tp"),
            P(None, "tp"),
            P("tp", "fs"),
            P("rep", "fs"),
        ),
        out_specs=(
            P(("rep", "fs"), "tp"),
            P(("rep", "fs"), "tp"),
            P(None, "tp"),
            P(None, "tp"),
            P("fs", "rep", "tp"),
            P("tp"),
        ),
        check_vma=False,
    )
```

```python
import functools

import jax
import jax.numpy as jnp
from jax import lax
from jax.experimental import pallas as pl
from jax.experimental.pallas import tpu as pltpu
from jax.sharding import PartitionSpec as P

MESH = pl.DeviceIdType.MESH
LANES = 128


def passed_along(array, axis, by):
    count = lax.axis_size(axis)
    pairs = [(i, i + by) for i in range(count) if 0 <= i + by < count]
    return lax.ppermute(array, axis, pairs)


def shift_conv(padded, tap_coef):
    return tap_coef[0] * padded[:-2] + tap_coef[1] * padded[1:-1] + tap_coef[2] * padded[2:]


def back_conv(padded, tap_coef):
    return tap_coef[2] * padded[:-2] + tap_coef[1] * padded[1:-1] + tap_coef[0] * padded[2:]


def local(gate_pre, up_pre, gate_taps, up_taps, down_weight, cotangent):
    tok_rows = gate_pre.shape[0]
    width = gate_pre.shape[1]
    prev_rows = passed_along(jnp.stack([gate_pre[-2:], up_pre[-2:]]), "fs", 1)
    gate_pad = jnp.concatenate([prev_rows[0], gate_pre], 0).astype(jnp.float32)
    up_pad = jnp.concatenate([prev_rows[1], up_pre], 0).astype(jnp.float32)
    gate_coef = gate_taps.astype(jnp.float32)
    up_coef = up_taps.astype(jnp.float32)
    gate_conv = shift_conv(gate_pad, gate_coef)
    up_conv = shift_conv(up_pad, up_coef)
    gate_sig = jax.nn.sigmoid(gate_conv)
    activated = gate_conv * gate_sig
    hidden = (activated * up_conv).astype(jnp.bfloat16)
    partial_rows = lax.dot_general(
        cotangent, down_weight, (((1,), (1,)), ((), ())), preferred_element_type=jnp.float32
    ).astype(jnp.bfloat16)
    received = lax.all_to_all(partial_rows, "fs", split_axis=0, concat_axis=0, tiled=True)
    d_hidden = jnp.sum(received.reshape(-1, tok_rows, width).astype(jnp.float32), axis=0)
    d_gate = d_hidden * up_conv * gate_sig * (1.0 + gate_conv * (1.0 - gate_sig))
    d_up = d_hidden * activated
    next_rows = passed_along(jnp.stack([d_gate[:2], d_up[:2]]), "fs", -1)
    grad_gate = back_conv(jnp.concatenate([d_gate, next_rows[0]], 0), gate_coef).astype(
        jnp.bfloat16
    )
    grad_up = back_conv(jnp.concatenate([d_up, next_rows[1]], 0), up_coef).astype(jnp.bfloat16)
    taps_part = jnp.stack(
        [
            jnp.stack(
                [
                    jnp.sum(d_gate * gate_pad[offset : offset + tok_rows], axis=0)
                    for offset in range(3)
                ]
            ),
            jnp.stack(
                [jnp.sum(d_up * up_pad[offset : offset + tok_rows], axis=0) for offset in range(3)]
            ),
        ]
    )
    grad_scale = float(tok_rows * lax.axis_size("rep") * lax.axis_size("fs")) ** (-0.5)
    folded_sum = lax.dot_general(
        cotangent,
        lax.all_gather(hidden, "fs", axis=0, tiled=True),
        (((0,), (0,)), ((), ())),
        preferred_element_type=jnp.float32,
    )
    grad_share = lax.psum_scatter(folded_sum, "rep", scatter_dimension=0, tiled=True)
    grad_share = grad_share * grad_scale
    norm_part = jnp.sum(grad_share * grad_share, axis=0)
    norm_total, taps_total = lax.psum((norm_part, taps_part), ("rep", "fs"))
    return (
        grad_gate,
        grad_up,
        taps_total[0] * grad_scale,
        taps_total[1] * grad_scale,
        grad_share[None],
        norm_total / (cotangent.shape[1] * lax.axis_size("fs")),
    )


HALO = 16
FS_MASKS = ((1, 2), (2, 1))
REP_MASKS = ((1, 2), (1, 2))


def flip(v, mask):
    if mask == 1:
        return v + 1 - 2 * (v % 2)
    if mask == 2:
        return (v + 2) % 4
    return 3 - v


def column_chunks(width):
    tiles = width // LANES
    sides = (tiles - tiles // 2, tiles // 2)
    chunks = [None] * 8
    at = 0
    for side, count in enumerate(sides):
        middle = count - 2
        for i, size in enumerate((1, middle - middle // 2, middle // 2, 1)):
            chunks[2 * i + side] = (at * LANES, size * LANES)
            at += size
    return chunks, sides[0] * LANES


def kernel(
    scale, model_width, gate_hbm, up_hbm, gtaps_hbm, utaps_hbm, weight_hbm, cot_hbm,
    gg_hbm, gu_hbm, gtaps_out, utaps_out, gd_hbm, norms_out,
    gate, up, gtaps, utaps, weight, cot, cot_t, halo_out, halo, gate_pad, up_pad, coef_gate, coef_up,
    hid, parts, rs1, rs2, rs_out, prod, prod_out, zs1, zs2, z_out, dg_pad, du_pad,
    dhalo_out, dhalo_in, taps_out1, taps_in1, taps_out2, taps_in2,
    norm_out1, norm_in1, norm_out2, norm_in2, grad_gate, grad_up, grad_down, load_sem, store_sem, send_sem, recv_sem,
):
    f = lax.axis_index("fs")
    r = lax.axis_index("rep")
    rows, width = gate.shape
    blk = grad_down.shape[0]
    chunks, split = column_chunks(width)
    n = len(chunks)
    sends = []

    loads = []
    for i, (src, dst) in enumerate((
        (gate_hbm, gate), (up_hbm, up), (cot_hbm, cot), (weight_hbm, weight),
        (gtaps_hbm, gtaps), (utaps_hbm, utaps),
    )):
        copy = pltpu.make_async_copy(src, dst, load_sem.at[i])
        copy.start()
        loads.append(copy)

    barrier = pltpu.get_barrier_semaphore()
    for d in (1, 2, 3):
        pl.semaphore_signal(barrier, inc=1, device_id={"fs": (f + d) % 4}, device_id_type=MESH)
        pl.semaphore_signal(barrier, inc=1, device_id={"rep": (r + d) % 4}, device_id_type=MESH)

    def push(src, dst, axis, to):
        k = len(sends)
        copy = pltpu.make_async_remote_copy(
            src_ref=src, dst_ref=dst, send_sem=send_sem.at[k], recv_sem=recv_sem.at[k],
            device_id={axis: to}, device_id_type=MESH,
        )
        copy.start()
        sends.append(copy)
        return copy

    def cols(c):
        return pl.ds(chunks[c][0], chunks[c][1])

    def tile_list(c):
        return [pl.ds(at, LANES) for at in range(chunks[c][0], chunks[c][0] + chunks[c][1], LANES)]

    def part(c):
        product = lax.dot_general(
            cot[...], weight[cols(c), :], (((1,), (1,)), ((), ())),
            preferred_element_type=jnp.float32,
        )
        parts[:, :, cols(c)] = product.astype(jnp.bfloat16).reshape(4, rows, chunks[c][1])

    rs1_in, rs2_in, ag1_in, ag2_in, z1_in, z2_in = {}, {}, {}, {}, {}, {}

    def rs_first(c):
        m1, m2 = FS_MASKS[c % 2]
        to = flip(f, m1)
        rs1_in[c] = [
            push(parts.at[flip(to, m2), :, cols(c)], rs1.at[1, :, cols(c)], "fs", to),
            push(parts.at[to, :, cols(c)], rs1.at[0, :, cols(c)], "fs", to),
        ]

    def rs_second(c):
        m1, m2 = FS_MASKS[c % 2]
        to = flip(f, m2)
        rs1_in[c][0].wait_recv()
        for t in tile_list(c):
            rs_out[:, t] = (
                parts[to, :, t].astype(jnp.float32) + rs1[1, :, t].astype(jnp.float32)
            ).astype(jnp.bfloat16)
        rs2_in[c] = push(rs_out.at[:, cols(c)], rs2.at[:, cols(c)], "fs", to)

    def activate(t, top, count):
        gc = [gtaps[k : k + 1, t].astype(jnp.float32) for k in range(3)]
        uc = [utaps[k : k + 1, t].astype(jnp.float32) for k in range(3)]
        g_conv = sum(gc[k] * gate_pad[pl.ds(top + 6 + k, count), t] for k in range(3))
        u_conv = sum(uc[k] * up_pad[pl.ds(top + 6 + k, count), t] for k in range(3))
        sig = jax.nn.sigmoid(g_conv)
        act = g_conv * sig
        at = pl.ds(top, count)
        hid[f, at, t] = (act * u_conv).astype(jnp.bfloat16)
        coef_up[at, t] = act
        coef_gate[at, t] = u_conv * sig * (1.0 + g_conv * (1.0 - sig))

    lower = pl.ds(HALO, rows - HALO)

    def pass_on(slot, row_range, col_range, to):
        ref = hid.at[slot, row_range, col_range]
        return push(ref, ref, "fs", to)

    def ag_first(c):
        ag1_in[c] = pass_on(f, lower, cols(c), flip(f, FS_MASKS[c % 2][0]))

    def ag_second(c):
        m1, m2 = FS_MASKS[c % 2]
        to = flip(f, m2)
        own = pass_on(f, lower, cols(c), to)
        ag1_in[c].wait_recv()
        ag2_in[c] = [own, pass_on(flip(f, m1), lower, cols(c), to)]

    upper = pl.ds(0, HALO)
    side_cols = (pl.ds(0, split), pl.ds(split, width - split))

    def top_first():
        return [pass_on(f, upper, side_cols[i], flip(f, FS_MASKS[i][0])) for i in range(2)]

    def top_second(first):
        out = []
        for i, (m1, m2) in enumerate(FS_MASKS):
            out.append(pass_on(f, upper, side_cols[i], flip(f, m2)))
            first[i].wait_recv()
            out.append(pass_on(flip(f, m1), upper, side_cols[i], flip(f, m2)))
        return out

    def product(c):
        for copy in ag2_in[c]:
            copy.wait_recv()
        result = jnp.dot(
            cot_t[...], hid[:, :, cols(c)].reshape(4 * rows, chunks[c][1]),
            preferred_element_type=jnp.float32,
        ).reshape(4, blk, chunks[c][1])
        prod[:, :, cols(c)] = result
        prod_out[:, :, cols(c)] = result.astype(jnp.bfloat16)
        m1, m2 = REP_MASKS[c % 2]
        to = flip(r, m1)
        z1_in[c] = [
            push(prod_out.at[flip(to, m2), :, cols(c)], zs1.at[1, :, cols(c)], "rep", to),
            push(prod_out.at[to, :, cols(c)], zs1.at[0, :, cols(c)], "rep", to),
        ]

    def z_second(c):
        m1, m2 = REP_MASKS[c % 2]
        to = flip(r, m2)
        z1_in[c][0].wait_recv()
        for t in tile_list(c):
            z_out[:, t] = (prod[to, :, t] + zs1[1, :, t].astype(jnp.float32)).astype(jnp.bfloat16)
        z2_in[c] = push(z_out.at[:, cols(c)], zs2.at[:, cols(c)], "rep", to)

    def z_last(c):
        z1_in[c][1].wait_recv()
        z2_in[c].wait_recv()
        for t in tile_list(c):
            total = (
                prod[r, :, t] + zs1[0, :, t].astype(jnp.float32) + zs2[:, t].astype(jnp.float32)
            ) * scale
            grad_down[:, t] = total
            norm_out1[:, t] = jnp.sum(total * total, axis=0, keepdims=True)

    def rs_last(c):
        rs1_in[c][1].wait_recv()
        rs2_in[c].wait_recv()
        for t in tile_list(c):
            dh = (
                parts[f, :, t].astype(jnp.float32)
                + rs1[0, :, t].astype(jnp.float32)
                + rs2[:, t].astype(jnp.float32)
            )
            d_gate = dh * coef_gate[:, t]
            d_up = dh * coef_up[:, t]
            dg_pad[pl.ds(0, rows), t] = d_gate
            du_pad[pl.ds(0, rows), t] = d_up
            dhalo_out[0:2, t] = d_gate[0:2]
            dhalo_out[2:4, t] = d_up[0:2]
            for k in range(3):
                taps_out1[k : k + 1, t] = jnp.sum(
                    d_gate * gate_pad[pl.ds(6 + k, rows), t], axis=0, keepdims=True
                )
                taps_out1[3 + k : 4 + k, t] = jnp.sum(
                    d_up * up_pad[pl.ds(6 + k, rows), t], axis=0, keepdims=True
                )

    def spread(src, landing, axis, me):
        return [push(src, landing.at[me], axis, (me + d) % 4) for d in (1, 2, 3)]

    def gather_sum(copies, own, landing, me):
        for copy in copies:
            copy.wait_recv()
        landing[me] = own[...]
        return (landing[0] + landing[1]) + (landing[2] + landing[3])

    for i in (0, 1, 4, 5):
        loads[i].wait()
    gate_pad[pl.ds(8, rows), :] = gate[...].astype(jnp.float32)
    up_pad[pl.ds(8, rows), :] = up[...].astype(jnp.float32)
    halo_out[0:2, :] = gate_pad[rows + 6 : rows + 8, :].astype(jnp.bfloat16)
    halo_out[2:4, :] = up_pad[rows + 6 : rows + 8, :].astype(jnp.bfloat16)
    taps_out1[...] = jnp.zeros_like(taps_out1)
    dhalo_out[...] = jnp.zeros_like(dhalo_out)
    for c in range(n):
        for t in tile_list(c):
            activate(t, HALO, rows - HALO)
    pl.semaphore_wait(barrier, 6)
    halo_in = push(halo_out, halo, "fs", (f + 1) % 4)
    ag_first(0)
    ag_first(1)
    ag_first(2)
    ag_first(3)
    loads[2].wait()
    loads[3].wait()
    part(0)
    part(1)
    halo_in.wait_recv()
    edge = halo[...].astype(jnp.float32) * (f > 0).astype(jnp.float32)
    gate_pad[6:8, :] = edge[0:2]
    up_pad[6:8, :] = edge[2:4]
    for c in range(n):
        for t in tile_list(c):
            activate(t, 0, HALO)
    top1 = top_first()
    ag_first(4)
    ag_first(5)
    ag_second(0)
    ag_second(1)
    ag_first(6)
    ag_first(7)
    top2 = top_second(top1)
    cot_t[...] = cot[...].T
    rs_first(0)
    rs_first(1)
    ag_second(2)
    ag_second(3)
    part(2)
    part(3)
    for copy in top2:
        copy.wait_recv()
    product(0)
    product(1)
    ag_second(4)
    ag_second(5)
    ag_second(6)
    ag_second(7)
    rs_first(2)
    rs_first(3)
    part(4)
    part(5)
    rs_first(4)
    rs_first(5)
    product(2)
    product(3)
    part(6)
    part(7)
    rs_first(6)
    rs_first(7)
    z_second(0)
    z_second(1)
    rs_second(0)
    rs_second(1)
    product(4)
    product(5)
    product(6)
    product(7)
    z_second(2)
    z_second(3)
    rs_second(2)
    rs_second(3)
    z_last(0)
    z_last(1)
    rs_last(0)
    rs_last(1)
    z_second(4)
    z_second(5)
    rs_second(4)
    rs_second(5)
    z_last(2)
    z_last(3)
    rs_last(2)
    rs_last(3)
    z_second(6)
    z_second(7)
    rs_second(6)
    rs_second(7)
    z_last(4)
    z_last(5)
    rs_last(4)
    rs_last(5)
    rs_last(6)
    rs_last(7)
    taps1 = spread(taps_out1, taps_in1, "fs", f)
    dhalo = push(dhalo_out, dhalo_in, "fs", (f + 3) % 4)
    z_last(6)
    z_last(7)
    store_down = pltpu.make_async_copy(grad_down, gd_hbm, store_sem.at[0])
    store_down.start()
    norm1 = spread(norm_out1, norm_in1, "fs", f)
    taps_out2[...] = gather_sum(taps1, taps_out1, taps_in1, f)
    taps2 = spread(taps_out2, taps_in2, "rep", r)
    norm_out2[...] = gather_sum(norm1, norm_out1, norm_in1, f)
    norm2 = spread(norm_out2, norm_in2, "rep", r)
    dhalo.wait_recv()
    inner = (f < 3).astype(jnp.float32)
    dg_pad[rows : rows + 2, :] = dhalo_in[0:2, :] * inner
    du_pad[rows : rows + 2, :] = dhalo_in[2:4, :] * inner
    for c in range(n):
        for t in tile_list(c):
            for taps, pad, out in ((gtaps, dg_pad, grad_gate), (utaps, du_pad, grad_up)):
                out[:, t] = sum(
                    taps[2 - k : 3 - k, t].astype(jnp.float32) * pad[pl.ds(k, rows), t]
                    for k in range(3)
                ).astype(jnp.bfloat16)
    stores = [store_down]
    for i, (src, dst) in enumerate(((grad_gate, gg_hbm), (grad_up, gu_hbm))):
        stores.append(pltpu.make_async_copy(src, dst, store_sem.at[1 + i]))
        stores[-1].start()
    taps_total = gather_sum(taps2, taps_out2, taps_in2, r) * scale
    gtaps_out[...] = taps_total[0:3]
    utaps_out[...] = taps_total[3:6]
    norms_out[...] = gather_sum(norm2, norm_out2, norm_in2, r) * (1.0 / model_width)
    for copy in stores:
        copy.wait()
    for copy in sends:
        copy.wait_send()


def hand_over(*refs):
    ins, outs, held, sems_in, sems_out = refs[:6], refs[6:12], refs[12:18], refs[18], refs[19]
    order = (4, 0, 1, 2, 3)
    fetch = {i: pltpu.make_async_copy(ins[i], held[i], sems_in.at[i]) for i in range(6)}
    store = {i: pltpu.make_async_copy(held[i], outs[i], sems_out.at[i]) for i in order}
    for i in (5,) + order:
        fetch[i].start()
    fetch[5].wait()
    outs[5][...] = held[5][0]
    for i in order:
        fetch[i].wait()
        store[i].start()
    for i in order:
        store[i].wait()


def fused(gate_pre, up_pre, gate_taps, up_taps, down_weight, cotangent):
    rows, width = gate_pre.shape
    if rows % 16 or width % LANES or width // LANES < 8 or cotangent.shape[1] % 64:
        return local(gate_pre, up_pre, gate_taps, up_taps, down_weight, cotangent)
    depth = cotangent.shape[1]
    blk = depth // lax.axis_size("rep")
    scale = float(rows * lax.axis_size("rep") * lax.axis_size("fs")) ** (-0.5)
    model_width = depth * lax.axis_size("fs")
    f32, bf16 = jnp.float32, jnp.bfloat16
    vmem = pltpu.VMEM
    shapes = [
        ((rows, width), bf16), ((rows, width), bf16), ((3, width), bf16), ((3, width), bf16),
        ((width, depth), bf16), ((4 * rows, depth), bf16), ((depth, 4 * rows), bf16),
        ((4, width), bf16), ((4, width), bf16), ((rows + 8, width), f32), ((rows + 8, width), f32),
        ((rows, width), f32), ((rows, width), f32),
        ((4, rows, width), bf16), ((4, rows, width), bf16), ((2, rows, width), bf16),
        ((rows, width), bf16), ((rows, width), bf16),
        ((4, blk, width), f32), ((4, blk, width), bf16), ((2, blk, width), bf16),
        ((blk, width), bf16), ((blk, width), bf16), ((rows + 8, width), f32),
        ((rows + 8, width), f32), ((8, width), f32), ((8, width), f32),
        ((8, width), f32), ((4, 8, width), f32), ((8, width), f32), ((4, 8, width), f32),
        ((1, width), f32), ((4, 1, width), f32), ((1, width), f32), ((4, 1, width), f32),
        ((rows, width), bf16), ((rows, width), bf16), ((blk, width), f32),
    ]
    outs = pl.pallas_call(
        functools.partial(kernel, scale, model_width),
        out_shape=[
            jax.ShapeDtypeStruct((rows, width), bf16), jax.ShapeDtypeStruct((rows, width), bf16),
            jax.ShapeDtypeStruct((3, width), f32), jax.ShapeDtypeStruct((3, width), f32),
            jax.ShapeDtypeStruct((blk, width), f32), jax.ShapeDtypeStruct((1, width), f32),
        ],
        in_specs=[pl.BlockSpec(memory_space=pl.ANY)] * 6,
        out_specs=[
            pl.BlockSpec(memory_space=pl.ANY if i in (0, 1, 4) else pltpu.VMEM) for i in range(6)
        ],
        scratch_shapes=[vmem(shape, kind) for shape, kind in shapes] + [
            pltpu.SemaphoreType.DMA((6,)), pltpu.SemaphoreType.DMA((3,)),
            pltpu.SemaphoreType.DMA((96,)),
            pltpu.SemaphoreType.DMA((96,)),
        ],
        compiler_params=pltpu.CompilerParams(
            collective_id=0, has_side_effects=True, vmem_limit_bytes=56 * 1024 * 1024
        ),
    )(gate_pre, up_pre, gate_taps, up_taps, down_weight, cotangent)
    final = pl.pallas_call(
        hand_over,
        out_shape=[jax.ShapeDtypeStruct(x.shape, x.dtype) for x in outs[:5]]
        + [jax.ShapeDtypeStruct((width,), f32)],
        in_specs=[pl.BlockSpec(memory_space=pl.ANY)] * 6,
        out_specs=[pl.BlockSpec(memory_space=pl.ANY)] * 5 + [pl.BlockSpec(memory_space=pltpu.VMEM)],
        scratch_shapes=[vmem(x.shape, x.dtype) for x in outs]
        + [pltpu.SemaphoreType.DMA((6,)), pltpu.SemaphoreType.DMA((6,))],
        compiler_params=pltpu.CompilerParams(vmem_limit_bytes=56 * 1024 * 1024),
    )(*outs)
    return final[0], final[1], final[2], final[3], final[4][None], final[5]


def solution(mesh):
    return jax.shard_map(
        fused if mesh.shape["fs"] == 4 and mesh.shape["rep"] == 4 else local,
        mesh=mesh,
        in_specs=(
            P(("rep", "fs"), "tp"),
            P(("rep", "fs"), "tp"),
            P(None, "tp"),
            P(None, "tp"),
            P("tp", "fs"),
            P("rep", "fs"),
        ),
        out_specs=(
            P(("rep", "fs"), "tp"),
            P(("rep", "fs"), "tp"),
            P(None, "tp"),
            P(None, "tp"),
            P("fs", "rep", "tp"),
            P("tp"),
        ),
        check_vma=False,
    )
```

```python
import functools

import jax
import jax.numpy as jnp
from jax import lax
from jax.experimental import pallas as pl
from jax.experimental.pallas import tpu as pltpu
from jax.sharding import PartitionSpec as P

MESH = pl.DeviceIdType.MESH
LANES = 128


def passed_along(array, axis, by):
    count = lax.axis_size(axis)
    pairs = [(i, i + by) for i in range(count) if 0 <= i + by < count]
    return lax.ppermute(array, axis, pairs)


def shift_conv(padded, tap_coef):
    return tap_coef[0] * padded[:-2] + tap_coef[1] * padded[1:-1] + tap_coef[2] * padded[2:]


def back_conv(padded, tap_coef):
    return tap_coef[2] * padded[:-2] + tap_coef[1] * padded[1:-1] + tap_coef[0] * padded[2:]


def local(gate_pre, up_pre, gate_taps, up_taps, down_weight, cotangent):
    tok_rows = gate_pre.shape[0]
    width = gate_pre.shape[1]
    prev_rows = passed_along(jnp.stack([gate_pre[-2:], up_pre[-2:]]), "fs", 1)
    gate_pad = jnp.concatenate([prev_rows[0], gate_pre], 0).astype(jnp.float32)
    up_pad = jnp.concatenate([prev_rows[1], up_pre], 0).astype(jnp.float32)
    gate_coef = gate_taps.astype(jnp.float32)
    up_coef = up_taps.astype(jnp.float32)
    gate_conv = shift_conv(gate_pad, gate_coef)
    up_conv = shift_conv(up_pad, up_coef)
    gate_sig = jax.nn.sigmoid(gate_conv)
    activated = gate_conv * gate_sig
    hidden = (activated * up_conv).astype(jnp.bfloat16)
    partial_rows = lax.dot_general(
        cotangent, down_weight, (((1,), (1,)), ((), ())), preferred_element_type=jnp.float32
    ).astype(jnp.bfloat16)
    received = lax.all_to_all(partial_rows, "fs", split_axis=0, concat_axis=0, tiled=True)
    d_hidden = jnp.sum(received.reshape(-1, tok_rows, width).astype(jnp.float32), axis=0)
    d_gate = d_hidden * up_conv * gate_sig * (1.0 + gate_conv * (1.0 - gate_sig))
    d_up = d_hidden * activated
    next_rows = passed_along(jnp.stack([d_gate[:2], d_up[:2]]), "fs", -1)
    grad_gate = back_conv(jnp.concatenate([d_gate, next_rows[0]], 0), gate_coef).astype(
        jnp.bfloat16
    )
    grad_up = back_conv(jnp.concatenate([d_up, next_rows[1]], 0), up_coef).astype(jnp.bfloat16)
    taps_part = jnp.stack(
        [
            jnp.stack(
                [
                    jnp.sum(d_gate * gate_pad[offset : offset + tok_rows], axis=0)
                    for offset in range(3)
                ]
            ),
            jnp.stack(
                [jnp.sum(d_up * up_pad[offset : offset + tok_rows], axis=0) for offset in range(3)]
            ),
        ]
    )
    grad_scale = float(tok_rows * lax.axis_size("rep") * lax.axis_size("fs")) ** (-0.5)
    folded_sum = lax.dot_general(
        cotangent,
        lax.all_gather(hidden, "fs", axis=0, tiled=True),
        (((0,), (0,)), ((), ())),
        preferred_element_type=jnp.float32,
    )
    grad_share = lax.psum_scatter(folded_sum, "rep", scatter_dimension=0, tiled=True)
    grad_share = grad_share * grad_scale
    norm_part = jnp.sum(grad_share * grad_share, axis=0)
    norm_total, taps_total = lax.psum((norm_part, taps_part), ("rep", "fs"))
    return (
        grad_gate,
        grad_up,
        taps_total[0] * grad_scale,
        taps_total[1] * grad_scale,
        grad_share[None],
        norm_total / (cotangent.shape[1] * lax.axis_size("fs")),
    )


HALO = 16
FS_MASKS = ((1, 2), (2, 1))
REP_MASKS = ((1, 2), (1, 2))


def flip(v, mask):
    if mask == 1:
        return v + 1 - 2 * (v % 2)
    if mask == 2:
        return (v + 2) % 4
    return 3 - v


def column_chunks(width):
    tiles = width // LANES
    sides = (tiles - tiles // 2, tiles // 2)
    chunks = [None] * 8
    at = 0
    for side, count in enumerate(sides):
        middle = count - 2
        for i, size in enumerate((1, middle - middle // 2, middle // 2, 1)):
            chunks[2 * i + side] = (at * LANES, size * LANES)
            at += size
    return chunks, sides[0] * LANES


def kernel(
    scale, model_width, gate_hbm, up_hbm, gtaps_hbm, utaps_hbm, weight_hbm, cot_hbm,
    gg_hbm, gu_hbm, gtaps_out, utaps_out, gd_hbm, norms_out,
    gate, up, gtaps, utaps, weight, cot, cot_t, edge, edges, edge_pad, patch, gate_pad, up_pad, coef_gate, coef_up,
    hid, parts, rs1, rs2, rs_out, prod, prod_out, zs1, zs2, z_out, dg_pad, du_pad,
    dhalo_out, dhalo_in, taps_out1, taps_in1, taps_out2, taps_in2,
    norm_out1, norm_in1, norm_out2, norm_in2, grad_gate, grad_up, grad_down, load_sem, store_sem, send_sem, recv_sem,
):
    f = lax.axis_index("fs")
    r = lax.axis_index("rep")
    rows, width = gate.shape
    blk = grad_down.shape[0]
    chunks, split = column_chunks(width)
    n = len(chunks)
    sends = []

    loads = []
    for i, (src, dst) in enumerate((
        (gate_hbm, gate), (up_hbm, up), (cot_hbm, cot), (weight_hbm, weight),
        (gtaps_hbm, gtaps), (utaps_hbm, utaps),
    )):
        copy = pltpu.make_async_copy(src, dst, load_sem.at[i])
        copy.start()
        loads.append(copy)

    barrier = pltpu.get_barrier_semaphore()
    for d in (1, 2, 3):
        pl.semaphore_signal(barrier, inc=1, device_id={"fs": (f + d) % 4}, device_id_type=MESH)
        pl.semaphore_signal(barrier, inc=1, device_id={"rep": (r + d) % 4}, device_id_type=MESH)

    def push(src, dst, axis, to):
        k = len(sends)
        copy = pltpu.make_async_remote_copy(
            src_ref=src, dst_ref=dst, send_sem=send_sem.at[k], recv_sem=recv_sem.at[k],
            device_id={axis: to}, device_id_type=MESH,
        )
        copy.start()
        sends.append(copy)
        return copy

    def cols(c):
        return pl.ds(chunks[c][0], chunks[c][1])

    def tile_list(c):
        return [pl.ds(at, LANES) for at in range(chunks[c][0], chunks[c][0] + chunks[c][1], LANES)]

    def part(c):
        product = lax.dot_general(
            cot[...], weight[cols(c), :], (((1,), (1,)), ((), ())),
            preferred_element_type=jnp.float32,
        )
        parts[:, :, cols(c)] = product.astype(jnp.bfloat16).reshape(4, rows, chunks[c][1])

    rs1_in, rs2_in, ag1_in, ag2_in, z1_in, z2_in = {}, {}, {}, {}, {}, {}

    def rs_first(c):
        m1, m2 = FS_MASKS[c % 2]
        to = flip(f, m1)
        rs1_in[c] = [
            push(parts.at[flip(to, m2), :, cols(c)], rs1.at[1, :, cols(c)], "fs", to),
            push(parts.at[to, :, cols(c)], rs1.at[0, :, cols(c)], "fs", to),
        ]

    def rs_second(c):
        m1, m2 = FS_MASKS[c % 2]
        to = flip(f, m2)
        rs1_in[c][0].wait_recv()
        for t in tile_list(c):
            rs_out[:, t] = (
                parts[to, :, t].astype(jnp.float32) + rs1[1, :, t].astype(jnp.float32)
            ).astype(jnp.bfloat16)
        rs2_in[c] = push(rs_out.at[:, cols(c)], rs2.at[:, cols(c)], "fs", to)

    def activation(t, top, count):
        gc = [gtaps[k : k + 1, t].astype(jnp.float32) for k in range(3)]
        uc = [utaps[k : k + 1, t].astype(jnp.float32) for k in range(3)]
        g_conv = sum(gc[k] * gate_pad[pl.ds(top + 6 + k, count), t] for k in range(3))
        u_conv = sum(uc[k] * up_pad[pl.ds(top + 6 + k, count), t] for k in range(3))
        sig = jax.nn.sigmoid(g_conv)
        act = g_conv * sig
        return act, u_conv * sig * (1.0 + g_conv * (1.0 - sig)), act * u_conv

    def activate(t):
        act, slope, rows_out = activation(t, 0, rows)
        row = lax.broadcasted_iota(jnp.int32, rows_out.shape, 0)
        hid[f, :, t] = jnp.where(row < 2, 0.0, rows_out).astype(jnp.bfloat16)
        coef_up[:, t] = act
        coef_gate[:, t] = slope

    def pass_on(slot, c, to):
        ref = hid.at[slot, :, cols(c)]
        return push(ref, ref, "fs", to)

    def ag_first(c):
        ag1_in[c] = pass_on(f, c, flip(f, FS_MASKS[c % 2][0]))

    def ag_second(c):
        m1, m2 = FS_MASKS[c % 2]
        to = flip(f, m2)
        own = pass_on(f, c, to)
        ag1_in[c].wait_recv()
        ag2_in[c] = [own, pass_on(flip(f, m1), c, to)]

    def edge_rows(incoming):
        for copy in incoming:
            copy.wait_recv()
        edges[f] = edge[...]
        patch[...] = jnp.zeros_like(patch)
        for slot in range(4):
            here = edges[slot].astype(jnp.float32)
            before = edges[slot - 1].astype(jnp.float32) if slot else jnp.zeros_like(here)
            for i in range(2):
                edge_pad[i, slot, 0:2, :] = before[4 + 2 * i : 6 + 2 * i]
                edge_pad[i, slot, 2:4, :] = here[2 * i : 2 * i + 2]
        for c in range(n):
            for t in tile_list(c):
                gc = [gtaps[k : k + 1, t].astype(jnp.float32) for k in range(3)]
                uc = [utaps[k : k + 1, t].astype(jnp.float32) for k in range(3)]
                g_conv = sum(gc[k] * edge_pad[0, :, k : k + 2, t] for k in range(3))
                u_conv = sum(uc[k] * edge_pad[1, :, k : k + 2, t] for k in range(3))
                patch[:, 0:2, t] = (g_conv * jax.nn.sigmoid(g_conv) * u_conv).astype(jnp.bfloat16)
        gate_pad[6:8, :] = edge_pad[0, f, 0:2, :]
        up_pad[6:8, :] = edge_pad[1, f, 0:2, :]
        for c in range(n):
            for t in tile_list(c):
                act, slope, _ = activation(t, 0, 8)
                coef_up[0:8, t] = act
                coef_gate[0:8, t] = slope

    def product(c):
        for copy in ag2_in[c]:
            copy.wait_recv()
        block = jnp.concatenate(
            [hid[:, 0:HALO, cols(c)] + patch[:, :, cols(c)], hid[:, HALO:, cols(c)]], axis=1
        )
        result = jnp.dot(
            cot_t[...], block.reshape(4 * rows, chunks[c][1]),
            preferred_element_type=jnp.float32,
        ).reshape(4, blk, chunks[c][1])
        prod[:, :, cols(c)] = result
        prod_out[:, :, cols(c)] = result.astype(jnp.bfloat16)
        m1, m2 = REP_MASKS[c % 2]
        to = flip(r, m1)
        z1_in[c] = [
            push(prod_out.at[flip(to, m2), :, cols(c)], zs1.at[1, :, cols(c)], "rep", to),
            push(prod_out.at[to, :, cols(c)], zs1.at[0, :, cols(c)], "rep", to),
        ]

    def z_second(c):
        m1, m2 = REP_MASKS[c % 2]
        to = flip(r, m2)
        z1_in[c][0].wait_recv()
        for t in tile_list(c):
            z_out[:, t] = (prod[to, :, t] + zs1[1, :, t].astype(jnp.float32)).astype(jnp.bfloat16)
        z2_in[c] = push(z_out.at[:, cols(c)], zs2.at[:, cols(c)], "rep", to)

    def z_last(c):
        z1_in[c][1].wait_recv()
        z2_in[c].wait_recv()
        for t in tile_list(c):
            total = (
                prod[r, :, t] + zs1[0, :, t].astype(jnp.float32) + zs2[:, t].astype(jnp.float32)
            ) * scale
            grad_down[:, t] = total
            norm_out1[:, t] = jnp.sum(total * total, axis=0, keepdims=True)

    def rs_last(c):
        rs1_in[c][1].wait_recv()
        rs2_in[c].wait_recv()
        for t in tile_list(c):
            dh = (
                parts[f, :, t].astype(jnp.float32)
                + rs1[0, :, t].astype(jnp.float32)
                + rs2[:, t].astype(jnp.float32)
            )
            d_gate = dh * coef_gate[:, t]
            d_up = dh * coef_up[:, t]
            dg_pad[pl.ds(0, rows), t] = d_gate
            du_pad[pl.ds(0, rows), t] = d_up
            dhalo_out[0:2, t] = d_gate[0:2]
            dhalo_out[2:4, t] = d_up[0:2]
            for k in range(3):
                taps_out1[k : k + 1, t] = jnp.sum(
                    d_gate * gate_pad[pl.ds(6 + k, rows), t], axis=0, keepdims=True
                )
                taps_out1[3 + k : 4 + k, t] = jnp.sum(
                    d_up * up_pad[pl.ds(6 + k, rows), t], axis=0, keepdims=True
                )

    def spread(src, landing, axis, me):
        return [push(src, landing.at[me], axis, (me + d) % 4) for d in (1, 2, 3)]

    def gather_sum(copies, own, landing, me):
        for copy in copies:
            copy.wait_recv()
        landing[me] = own[...]
        return (landing[0] + landing[1]) + (landing[2] + landing[3])

    for i in (0, 1, 4, 5):
        loads[i].wait()
    gate_pad[pl.ds(8, rows), :] = gate[...].astype(jnp.float32)
    up_pad[pl.ds(8, rows), :] = up[...].astype(jnp.float32)
    gate_pad[0:8, :] = jnp.zeros((8, width), jnp.float32)
    up_pad[0:8, :] = jnp.zeros((8, width), jnp.float32)
    for i, pad in enumerate((gate_pad, up_pad)):
        edge[2 * i : 2 * i + 2, :] = pad[8:10, :].astype(jnp.bfloat16)
        edge[4 + 2 * i : 6 + 2 * i, :] = pad[rows + 6 : rows + 8, :].astype(jnp.bfloat16)
    taps_out1[...] = jnp.zeros_like(taps_out1)
    dhalo_out[...] = jnp.zeros_like(dhalo_out)
    for c in range(n):
        for t in tile_list(c):
            activate(t)
    pl.semaphore_wait(barrier, 6)
    ag_first(0)
    ag_first(1)
    edge_in = spread(edge, edges, "fs", f)
    ag_first(2)
    ag_first(3)
    loads[2].wait()
    loads[3].wait()
    cot_t[...] = cot[...].T
    part(0)
    part(1)
    ag_second(0)
    ag_second(1)
    ag_first(4)
    ag_first(5)
    edge_rows(edge_in)
    part(2)
    part(3)
    ag_second(2)
    ag_second(3)
    ag_first(6)
    ag_first(7)
    product(0)
    product(1)
    ag_second(4)
    ag_second(5)
    rs_first(0)
    rs_first(1)
    part(4)
    part(5)
    product(2)
    product(3)
    ag_second(6)
    ag_second(7)
    z_second(0)
    z_second(1)
    rs_first(2)
    rs_first(3)
    rs_first(4)
    rs_first(5)
    part(6)
    part(7)
    rs_first(6)
    rs_first(7)
    product(4)
    product(5)
    rs_second(0)
    rs_second(1)
    product(6)
    product(7)
    z_second(2)
    z_second(3)
    z_last(0)
    z_last(1)
    rs_second(2)
    rs_second(3)
    z_second(4)
    z_second(5)
    rs_second(4)
    rs_second(5)
    z_second(6)
    z_second(7)
    rs_second(6)
    rs_second(7)
    rs_last(0)
    rs_last(1)
    rs_last(2)
    rs_last(3)
    z_last(2)
    z_last(3)
    rs_last(4)
    rs_last(5)
    z_last(4)
    z_last(5)
    rs_last(6)
    rs_last(7)
    taps1 = spread(taps_out1, taps_in1, "fs", f)
    dhalo = push(dhalo_out, dhalo_in, "fs", (f + 3) % 4)
    z_last(6)
    z_last(7)
    store_down = pltpu.make_async_copy(grad_down, gd_hbm, store_sem.at[0])
    store_down.start()
    norm1 = spread(norm_out1, norm_in1, "fs", f)
    taps_out2[...] = gather_sum(taps1, taps_out1, taps_in1, f)
    taps2 = spread(taps_out2, taps_in2, "rep", r)
    norm_out2[...] = gather_sum(norm1, norm_out1, norm_in1, f)
    norm2 = spread(norm_out2, norm_in2, "rep", r)
    dhalo.wait_recv()
    inner = (f < 3).astype(jnp.float32)
    dg_pad[rows : rows + 2, :] = dhalo_in[0:2, :] * inner
    du_pad[rows : rows + 2, :] = dhalo_in[2:4, :] * inner
    for c in range(n):
        for t in tile_list(c):
            for taps, pad, out in ((gtaps, dg_pad, grad_gate), (utaps, du_pad, grad_up)):
                out[:, t] = sum(
                    taps[2 - k : 3 - k, t].astype(jnp.float32) * pad[pl.ds(k, rows), t]
                    for k in range(3)
                ).astype(jnp.bfloat16)
    stores = [store_down]
    for i, (src, dst) in enumerate(((grad_gate, gg_hbm), (grad_up, gu_hbm))):
        stores.append(pltpu.make_async_copy(src, dst, store_sem.at[1 + i]))
        stores[-1].start()
    taps_total = gather_sum(taps2, taps_out2, taps_in2, r) * scale
    gtaps_out[...] = taps_total[0:3]
    utaps_out[...] = taps_total[3:6]
    norms_out[...] = gather_sum(norm2, norm_out2, norm_in2, r) * (1.0 / model_width)
    for copy in stores:
        copy.wait()
    for copy in sends:
        copy.wait_send()


def hand_over(*refs):
    ins, outs, held, sems_in, sems_out = refs[:6], refs[6:12], refs[12:18], refs[18], refs[19]
    order = (4, 0, 1, 2, 3)
    fetch = {i: pltpu.make_async_copy(ins[i], held[i], sems_in.at[i]) for i in range(6)}
    store = {i: pltpu.make_async_copy(held[i], outs[i], sems_out.at[i]) for i in order}
    for i in (5,) + order:
        fetch[i].start()
    fetch[5].wait()
    outs[5][...] = held[5][0]
    for i in order:
        fetch[i].wait()
        store[i].start()
    for i in order:
        store[i].wait()


def fused(gate_pre, up_pre, gate_taps, up_taps, down_weight, cotangent):
    rows, width = gate_pre.shape
    if rows % 16 or width % LANES or width // LANES < 8 or cotangent.shape[1] % 64:
        return local(gate_pre, up_pre, gate_taps, up_taps, down_weight, cotangent)
    depth = cotangent.shape[1]
    blk = depth // lax.axis_size("rep")
    scale = float(rows * lax.axis_size("rep") * lax.axis_size("fs")) ** (-0.5)
    model_width = depth * lax.axis_size("fs")
    f32, bf16 = jnp.float32, jnp.bfloat16
    vmem = pltpu.VMEM
    shapes = [
        ((rows, width), bf16), ((rows, width), bf16), ((3, width), bf16), ((3, width), bf16),
        ((width, depth), bf16), ((4 * rows, depth), bf16), ((depth, 4 * rows), bf16),
        ((8, width), bf16), ((4, 8, width), bf16),
        ((2, 4, 8, width), f32), ((4, HALO, width), bf16), ((rows + 8, width), f32), ((rows + 8, width), f32),
        ((rows, width), f32), ((rows, width), f32),
        ((4, rows, width), bf16), ((4, rows, width), bf16), ((2, rows, width), bf16),
        ((rows, width), bf16), ((rows, width), bf16),
        ((4, blk, width), f32), ((4, blk, width), bf16), ((2, blk, width), bf16),
        ((blk, width), bf16), ((blk, width), bf16), ((rows + 8, width), f32),
        ((rows + 8, width), f32), ((8, width), f32), ((8, width), f32),
        ((8, width), f32), ((4, 8, width), f32), ((8, width), f32), ((4, 8, width), f32),
        ((1, width), f32), ((4, 1, width), f32), ((1, width), f32), ((4, 1, width), f32),
        ((rows, width), bf16), ((rows, width), bf16), ((blk, width), f32),
    ]
    outs = pl.pallas_call(
        functools.partial(kernel, scale, model_width),
        out_shape=[
            jax.ShapeDtypeStruct((rows, width), bf16), jax.ShapeDtypeStruct((rows, width), bf16),
            jax.ShapeDtypeStruct((3, width), f32), jax.ShapeDtypeStruct((3, width), f32),
            jax.ShapeDtypeStruct((blk, width), f32), jax.ShapeDtypeStruct((1, width), f32),
        ],
        in_specs=[pl.BlockSpec(memory_space=pl.ANY)] * 6,
        out_specs=[
            pl.BlockSpec(memory_space=pl.ANY if i in (0, 1, 4) else pltpu.VMEM) for i in range(6)
        ],
        scratch_shapes=[vmem(shape, kind) for shape, kind in shapes] + [
            pltpu.SemaphoreType.DMA((6,)), pltpu.SemaphoreType.DMA((3,)),
            pltpu.SemaphoreType.DMA((96,)),
            pltpu.SemaphoreType.DMA((96,)),
        ],
        compiler_params=pltpu.CompilerParams(
            collective_id=0, has_side_effects=True, vmem_limit_bytes=56 * 1024 * 1024
        ),
    )(gate_pre, up_pre, gate_taps, up_taps, down_weight, cotangent)
    final = pl.pallas_call(
        hand_over,
        out_shape=[jax.ShapeDtypeStruct(x.shape, x.dtype) for x in outs[:5]]
        + [jax.ShapeDtypeStruct((width,), f32)],
        in_specs=[pl.BlockSpec(memory_space=pl.ANY)] * 6,
        out_specs=[pl.BlockSpec(memory_space=pl.ANY)] * 5 + [pl.BlockSpec(memory_space=pltpu.VMEM)],
        scratch_shapes=[vmem(x.shape, x.dtype) for x in outs]
        + [pltpu.SemaphoreType.DMA((6,)), pltpu.SemaphoreType.DMA((6,))],
        compiler_params=pltpu.CompilerParams(vmem_limit_bytes=56 * 1024 * 1024),
    )(*outs)
    return final[0], final[1], final[2], final[3], final[4][None], final[5]


def solution(mesh):
    return jax.shard_map(
        fused if mesh.shape["fs"] == 4 and mesh.shape["rep"] == 4 else local,
        mesh=mesh,
        in_specs=(
            P(("rep", "fs"), "tp"),
            P(("rep", "fs"), "tp"),
            P(None, "tp"),
            P(None, "tp"),
            P("tp", "fs"),
            P("rep", "fs"),
        ),
        out_specs=(
            P(("rep", "fs"), "tp"),
            P(("rep", "fs"), "tp"),
            P(None, "tp"),
            P(None, "tp"),
            P("fs", "rep", "tp"),
            P("tp"),
        ),
        check_vma=False,
    )
```
